32 devices in a mesh: row: 8 (over z, x), col: 4 (over y, core).
Axes of the slice: x: 2, y: 2, z: 4, core: 2. Of those that a mesh axis runs over, the one named last changes fastest.
Arguments:
- tokens: bfloat16 [16384, 4096], P(('row', 'col')), may hold values from -36 to 36
- norm_gain: bfloat16 [4096], replicated, may hold values from 0.099609375 to 1.8984375
- in_weight: bfloat16 [4096, 1024], replicated, may hold values from -0.09375 to 0.09375
- out_weight: bfloat16 [1024, 4096], replicated, may hold values from -0.1875 to 0.1875
Outputs:
- mixed: bfloat16 [16384, 4096], P(('row', 'col'))
The draws below stay inside these ranges and needn't reach their ends.
All inputs are finite; a program needn't handle non-finite values.
Results may differ from the reference program's by a relative error of at most 0.0071.
Values may be sent and summed in bfloat16 or wider, within the bound.
A program may use at most 128 MiB of HBM per device.

```python
import jax
import jax.numpy as jnp
from jax import lax

D = 4096
GROUP_WIDTH = 64
F = 1024
TOKENS = 16384


def draw_tokens(key, part):
    keys = jax.random.split(key, 3)
    base = jnp.clip(jax.random.normal(keys[0], (TOKENS, D), jnp.float32), -4.0, 4.0)
    row_scales = jnp.exp(jax.random.uniform(keys[1], (TOKENS, 1), jnp.float32, -1.2, 1.0986))
    col_scales = jnp.exp(jax.random.uniform(keys[2], (1, D), jnp.float32, -1.2, 1.0986))
    return (base * row_scales * col_scales).astype(jnp.bfloat16)


def scatter_about(rng, extent, spread, limit, held_as=jnp.bfloat16):
    return jnp.clip(spread * jax.random.normal(rng, extent, jnp.float32), -limit, limit).astype(held_as)


def setup_inputs(seed: int = 0) -> dict:
    streams_of = jax.random.split(jax.random.key(seed), 5)
    return {
        "tokens": draw_tokens(jax.random.fold_in(streams_of[4], 71), 0),
        "norm_gain": jnp.clip(1.0 + 0.18 * jax.random.normal(streams_of[1], (D,), jnp.float32), 0.099609375, 1.8984375).astype(jnp.bfloat16),
        "in_weight": scatter_about(streams_of[2], (D, F), D ** -0.5, 0.09375),
        "out_weight": scatter_about(streams_of[3], (F, D), F ** -0.5, 0.1875),
    }


def reference(tokens, norm_gain, in_weight, out_weight):
    floats = tokens.astype(jnp.float32)
    scaling = lax.rsqrt(lax.optimization_barrier(jnp.mean(floats * floats, axis=-1, keepdims=True)) + 1e-06)
    normed = (floats * scaling * norm_gain.astype(jnp.float32)).astype(jnp.bfloat16)
    hidden = jnp.dot(normed, in_weight, preferred_element_type=jnp.float32).astype(jnp.bfloat16)
    widened = lax.optimization_barrier(hidden).astype(jnp.float32)
    length = widened.shape[0]
    grouped = widened.reshape(length, widened.shape[1] // GROUP_WIDTH, GROUP_WIDTH)
    channel_spectrum = jnp.fft.fft(grouped, axis=2, norm='ortho')
    real_rounded = channel_spectrum.real.astype(jnp.bfloat16)
    imag_rounded = channel_spectrum.imag.astype(jnp.bfloat16)
    real_rounded, imag_rounded = lax.optimization_barrier((real_rounded, imag_rounded))
    combined = real_rounded.astype(jnp.float32) + 1j * imag_rounded.astype(jnp.float32)
    spectrum = jnp.fft.fft(combined, axis=0, norm='ortho').real
    spectrum = spectrum.reshape(length, widened.shape[1]).astype(jnp.bfloat16)
    return jnp.dot(spectrum, out_weight, preferred_element_type=jnp.float32).astype(jnp.bfloat16)
```

```python
import functools
import math

import jax
import jax.numpy as jnp
import numpy as np
from jax import lax
from jax.experimental import pallas as pl
from jax.experimental.pallas import tpu as pltpu
from jax.sharding import PartitionSpec as P

GROUP_WIDTH = 64
AXES = ("row", "col")


def channel_tables(slots):
    pairs = slots // 2
    half = GROUP_WIDTH // 2
    index = np.arange(GROUP_WIDTH)
    forward = np.zeros((GROUP_WIDTH, GROUP_WIDTH))
    order = np.zeros((GROUP_WIDTH, GROUP_WIDTH))
    for slot in range(GROUP_WIDTH):
        place, within = divmod(slot, slots)
        pair = place * pairs + within % pairs
        angles = 2.0 * math.pi / GROUP_WIDTH * (pair * index % GROUP_WIDTH)
        if within < pairs:
            forward[slot] = np.cos(angles)
            order[pair, slot] = 1.0
        elif pair == 0:
            forward[slot] = np.cos(math.pi * index)
            order[half, slot] = 1.0
        else:
            forward[slot] = np.sin(angles)
            order[GROUP_WIDTH - pair, slot] = 1.0
    forward /= math.sqrt(GROUP_WIDTH)
    return forward.astype(jnp.bfloat16), order.astype(jnp.bfloat16)


def position_tables(outer, inner):
    length = outer * inner
    k1 = np.arange(outer)
    n2 = np.arange(inner)
    one = 2.0 * math.pi / outer * (np.outer(k1, k1) % outer)
    first = np.concatenate([np.cos(one), -np.sin(one)], axis=1)
    turn = 2.0 * math.pi / length * np.outer(n2, k1)
    two = 2.0 * math.pi / inner * (np.outer(n2, n2) % inner)
    scale = 1.0 / math.sqrt(length)
    c, s, z = np.cos(two) * scale, np.sin(two) * scale, np.zeros((inner, inner))
    usual = np.block([[c, s, -s, c], [c, s, s, -c]])
    special = np.block([[c, s, z, z], [z, z, c, s]])
    return (
        first.astype(jnp.bfloat16),
        np.cos(turn).astype(np.float32),
        np.sin(turn).astype(np.float32),
        usual.astype(jnp.bfloat16),
        special.astype(jnp.bfloat16),
    )


def position_kernel(pairs, x_ref, first_ref, cos_ref, sin_ref, usual_ref, zeroth_ref, o_ref):
    outer = first_ref.shape[0]
    inner = cos_ref.shape[0]

    def turned(slot):
        a = lax.dot_general(
            x_ref[slot], first_ref[...], (((0,), (0,)), ((), ())), preferred_element_type=jnp.float32
        )
        re, im = a[:, :outer], a[:, outer:]
        c, s = cos_ref[...], sin_ref[...]
        return [(re * c + im * s).astype(jnp.bfloat16), (im * c - re * s).astype(jnp.bfloat16)]

    for pair in range(pairs):
        b = jnp.concatenate(turned(pair) + turned(pair + pairs), axis=0)
        table = zeroth_ref if pair == 0 else usual_ref
        o = jnp.dot(table[...], b, preferred_element_type=jnp.float32).astype(jnp.bfloat16)
        o_ref[pair] = o[:inner]
        o_ref[pair + pairs] = o[inner:]


def position_transform(x, zeroth_here, outer, inner):
    slots = x.shape[0]
    first, turn_cos, turn_sin, usual, special = position_tables(outer, inner)
    zeroth = jnp.where(zeroth_here, special, usual)
    return pl.pallas_call(
        functools.partial(position_kernel, slots // 2),
        out_shape=jax.ShapeDtypeStruct((slots, inner, outer), jnp.bfloat16),
        in_specs=[pl.BlockSpec(memory_space=pltpu.VMEM)] * 6,
        out_specs=pl.BlockSpec(memory_space=pltpu.VMEM),
    )(x, first, turn_cos, turn_sin, usual, zeroth)


def exchange(blocks):
    return lax.all_to_all(blocks, AXES, split_axis=0, concat_axis=0, tiled=True)


def local(tokens, norm_gain, in_weight, out_weight):
    rows_here = tokens.shape[0]
    channels = in_weight.shape[1]
    groups = channels // GROUP_WIDTH
    devices = lax.axis_size(AXES)
    me = lax.axis_index(AXES)
    slots = channels // devices
    length = rows_here * devices
    inner = 1 << ((length.bit_length()) // 2)
    outer = length // inner
    split = rows_here // inner

    forward, order = channel_tables(slots)
    floats = tokens.astype(jnp.float32)
    scaling = lax.rsqrt(jnp.mean(floats * floats, axis=-1, keepdims=True) + 1e-06)
    normed = (floats * scaling * norm_gain.astype(jnp.float32)).astype(jnp.bfloat16)
    hidden = lax.dot_general(
        in_weight, normed, (((0,), (1,)), ((), ())), preferred_element_type=jnp.float32
    ).astype(jnp.bfloat16)
    sent = jnp.einsum(
        "sc,gct->gst",
        forward,
        hidden.reshape(groups, GROUP_WIDTH, rows_here),
        preferred_element_type=jnp.float32,
    ).astype(jnp.bfloat16)
    taken = exchange(sent.reshape(devices, slots, rows_here))
    grid = taken.reshape(devices, slots, split, inner).transpose(1, 0, 2, 3)
    zeroth_here = me * (slots // 2) % (GROUP_WIDTH // 2) == 0
    done = position_transform(grid.reshape(slots, outer, inner), zeroth_here, outer, inner)
    back = done.reshape(slots, devices, rows_here // outer, outer).transpose(1, 0, 2, 3)
    returned = exchange(back.reshape(devices, slots, rows_here))
    ordered = jnp.einsum(
        "ms,gst->gmt",
        order,
        returned.reshape(groups, GROUP_WIDTH, rows_here),
        preferred_element_type=jnp.float32,
    ).astype(jnp.bfloat16)
    mixed = lax.dot_general(
        ordered.reshape(channels, rows_here),
        out_weight,
        (((0,), (0,)), ((), ())),
        preferred_element_type=jnp.float32,
    )
    return mixed.astype(jnp.bfloat16)


def solution(mesh):
    placed = (P(AXES, None), P(), P(), P())
    return jax.shard_map(
        local, mesh=mesh, in_specs=placed, out_specs=P(AXES, None), check_vma=False
    )
```

```python
import functools
import math

import jax
import jax.numpy as jnp
import numpy as np
from jax import lax
from jax.experimental import pallas as pl
from jax.experimental.pallas import tpu as pltpu
from jax.sharding import PartitionSpec as P

GROUP_WIDTH = 64
AXES = ("row", "col")


def channel_tables(slots):
    pairs = slots // 2
    half = GROUP_WIDTH // 2
    index = np.arange(GROUP_WIDTH)
    forward = np.zeros((GROUP_WIDTH, GROUP_WIDTH))
    order = np.zeros((GROUP_WIDTH, GROUP_WIDTH))
    for slot in range(GROUP_WIDTH):
        place, within = divmod(slot, slots)
        pair = place * pairs + within % pairs
        angles = 2.0 * math.pi / GROUP_WIDTH * (pair * index % GROUP_WIDTH)
        if within < pairs:
            forward[slot] = np.cos(angles)
            order[pair, slot] = 1.0
        elif pair == 0:
            forward[slot] = np.cos(math.pi * index)
            order[half, slot] = 1.0
        else:
            forward[slot] = np.sin(angles)
            order[GROUP_WIDTH - pair, slot] = 1.0
    forward /= math.sqrt(GROUP_WIDTH)
    return forward.astype(jnp.bfloat16), order.astype(jnp.bfloat16)


def position_tables(outer, inner):
    length = outer * inner
    k1 = np.arange(outer)
    n2 = np.arange(inner)
    one = 2.0 * math.pi / outer * (np.outer(k1, k1) % outer)
    first = np.concatenate([np.cos(one), -np.sin(one)], axis=1)
    turn = 2.0 * math.pi / length * np.outer(n2, k1)
    two = 2.0 * math.pi / inner * (np.outer(n2, n2) % inner)
    scale = 1.0 / math.sqrt(length)
    c, s, z = np.cos(two) * scale, np.sin(two) * scale, np.zeros((inner, inner))
    usual = np.block([[c, s, -s, c], [c, s, s, -c]])
    special = np.block([[c, s, z, z], [z, z, c, s]])
    return (
        first.astype(jnp.bfloat16),
        np.cos(turn).astype(np.float32),
        np.sin(turn).astype(np.float32),
        usual.astype(jnp.bfloat16),
        special.astype(jnp.bfloat16),
    )


def position_kernel(pairs, x_ref, first_ref, cos_ref, sin_ref, usual_ref, zeroth_ref, o_ref):
    outer = first_ref.shape[0]
    inner = cos_ref.shape[0]

    def turned(slot):
        a = lax.dot_general(
            x_ref[slot], first_ref[...], (((0,), (0,)), ((), ())), preferred_element_type=jnp.float32
        )
        re, im = a[:, :outer], a[:, outer:]
        c, s = cos_ref[...], sin_ref[...]
        return [(re * c + im * s).astype(jnp.bfloat16), (im * c - re * s).astype(jnp.bfloat16)]

    for pair in range(pairs):
        b = jnp.concatenate(turned(pair) + turned(pair + pairs), axis=0)
        table = zeroth_ref if pair == 0 else usual_ref
        o = jnp.dot(table[...], b, preferred_element_type=jnp.float32).astype(jnp.bfloat16)
        o_ref[pair] = o[:inner]
        o_ref[pair + pairs] = o[inner:]


def position_transform(x, zeroth_here, outer, inner):
    slots = x.shape[0]
    first, turn_cos, turn_sin, usual, special = position_tables(outer, inner)
    zeroth = jnp.where(zeroth_here, special, usual)
    return pl.pallas_call(
        functools.partial(position_kernel, slots // 2),
        out_shape=jax.ShapeDtypeStruct((slots, inner, outer), jnp.bfloat16),
        in_specs=[pl.BlockSpec(memory_space=pltpu.VMEM)] * 6,
        out_specs=pl.BlockSpec(memory_space=pltpu.VMEM),
    )(x, first, turn_cos, turn_sin, usual, zeroth)


PLANES = 4
MESH = pl.DeviceIdType.MESH


def place_of(device, columns):
    return (device // columns, device % columns)


def turned_plane(plane, step):
    high = (plane // 2 + 1 - step // 2) % 2
    low = (plane % 2 + (step + 1) // 2) % 2
    return 2 * high + low


def here(devices):
    columns = lax.axis_size("col")
    me = lax.axis_index("row") * columns + lax.axis_index("col")
    per = devices // PLANES
    return me, columns, per, me // per, me % per


def greet(devices):
    me, columns, _, _, _ = here(devices)
    barrier = pltpu.get_barrier_semaphore()

    def signal(step, carry):
        other = (me + step) % devices
        pl.semaphore_signal(barrier, inc=1, device_id=place_of(other, columns), device_id_type=MESH)
        return carry

    lax.fori_loop(1, devices, signal, 0)
    return lambda: pl.semaphore_wait(barrier, devices - 1)


def send_plane(devices, step, from_ref, to_ref, send_sem, recv_sem, first):
    me, columns, per, plane, lane = here(devices)
    target_plane = turned_plane(plane, step)

    def send(hop, carry):
        target = target_plane * per + (lane + hop) % per
        pltpu.make_async_remote_copy(
            src_ref=from_ref.at[target],
            dst_ref=to_ref.at[me],
            send_sem=send_sem.at[step],
            recv_sem=recv_sem.at[step],
            device_id=place_of(target, columns),
            device_id_type=MESH,
        ).start()
        return carry

    lax.fori_loop(first, per, send, 0)


def wait_for(ref, sem, count):
    part = ref.at[pl.ds(0, count)]
    pltpu.make_async_copy(part, part, sem).wait()


def enter_kernel(
    devices, tokens, gain, weight, forward, out, raw, normed, held, sent, token_sem, weight_sem, own_sem, send_sem, recv_sem
):
    me, columns, per, plane, lane = here(devices)
    pieces = token_sem.shape[0]
    rows = raw.shape[0]
    piece = rows // pieces
    width = held.shape[2]

    def token_copy(index):
        part = pl.ds(index * piece, piece)
        return pltpu.make_async_copy(tokens.at[part], raw.at[part], token_sem.at[index])

    def weight_copy(step):
        target_plane = turned_plane(plane, step)
        part = pl.ds(pl.multiple_of(target_plane * width, width), width)
        return pltpu.make_async_copy(weight.at[:, part], held.at[step], weight_sem.at[step])

    for index in range(pieces):
        token_copy(index).start()
    for step in range(PLANES):
        weight_copy(step).start()
    arrive = greet(devices)

    block = 16
    for index in range(pieces):
        token_copy(index).wait()

        def normalise(number, carry):
            part = pl.ds(pl.multiple_of(index * piece + number * block, block), block)
            floats = raw[part, :].astype(jnp.float32)
            scaling = lax.rsqrt(jnp.mean(floats * floats, axis=-1, keepdims=True) + 1e-06)
            normed[part, :] = (floats * scaling * gain[...].astype(jnp.float32)).astype(jnp.bfloat16)
            return carry

        lax.fori_loop(0, piece // block, normalise, 0)

    arrive()

    def chunk(step, carry):
        weight_copy(step).wait()
        target_plane = turned_plane(plane, step)
        hidden = jnp.dot(normed[...], held[step], preferred_element_type=jnp.float32).astype(jnp.bfloat16)
        spectrum = lax.dot_general(
            forward[...], hidden, (((1,), (1,)), ((), ())), preferred_element_type=jnp.float32
        )
        sent[pl.ds(target_plane * per, per)] = spectrum.reshape(per, width // per, rows).astype(jnp.bfloat16)
        send_plane(devices, step, sent, out, send_sem, recv_sem, step // (PLANES - 1))
        return carry

    lax.fori_loop(0, PLANES, chunk, 0)
    own = pltpu.make_async_copy(sent.at[me], out.at[me], own_sem)
    own.start()
    finish(per, sent, send_sem)
    finish(per, sent, recv_sem)
    own.wait()


def finish(per, ref, sem):
    for step in range(PLANES):
        wait_for(ref, sem.at[step], per - step // (PLANES - 1))


def enter(tokens, gain, weight, forward, devices):
    rows, depth = tokens.shape
    channels = weight.shape[1]
    slots = channels // devices
    whole = pl.BlockSpec(memory_space=pltpu.VMEM)
    far = pl.BlockSpec(memory_space=pl.ANY)
    pieces = 4
    return pl.pallas_call(
        functools.partial(enter_kernel, devices),
        out_shape=jax.ShapeDtypeStruct((devices, slots, rows), jnp.bfloat16),
        in_specs=[far, whole, far, whole],
        out_specs=far,
        scratch_shapes=[
            pltpu.VMEM((rows, depth), jnp.bfloat16),
            pltpu.VMEM((rows, depth), jnp.bfloat16),
            pltpu.VMEM((PLANES, depth, channels // PLANES), jnp.bfloat16),
            pltpu.VMEM((devices, slots, rows), jnp.bfloat16),
            pltpu.SemaphoreType.DMA((pieces,)),
            pltpu.SemaphoreType.DMA((PLANES,)),
            pltpu.SemaphoreType.DMA,
            pltpu.SemaphoreType.DMA((PLANES,)),
            pltpu.SemaphoreType.DMA((PLANES,)),
        ],
        compiler_params=pltpu.CompilerParams(collective_id=0, has_side_effects=True, vmem_limit_bytes=40 << 20),
    )(tokens, gain.reshape(1, depth), weight, forward)


def leave_kernel(devices, back, order, out, taken, own_sem, send_sem, recv_sem):
    me, columns, per, plane, lane = here(devices)
    greet(devices)()
    for step in range(PLANES):
        send_plane(devices, step, back, taken, send_sem, recv_sem, step // (PLANES - 1))
    own = pltpu.make_async_copy(back.at[me], taken.at[me], own_sem)
    own.start()
    width = order.shape[0]
    rows = out.shape[0]
    own.wait()
    for number in range(PLANES):
        step = PLANES - 1 - number
        wait_for(taken, recv_sem.at[step], per - step // (PLANES - 1))
        source = turned_plane(plane, step)
        part = taken[pl.ds(source * per, per)].astype(jnp.float32).reshape(width, rows).astype(jnp.bfloat16)
        turned = lax.dot_general(
            part, order[...], (((0,), (0,)), ((), ())), preferred_element_type=jnp.float32
        ).astype(jnp.bfloat16)
        out[:, pl.ds(pl.multiple_of(source * width, width), width)] = turned
    finish(per, back, send_sem)


def leave(back, order, devices):
    _, slots, rows = back.shape
    whole = pl.BlockSpec(memory_space=pltpu.VMEM)
    far = pl.BlockSpec(memory_space=pl.ANY)
    return pl.pallas_call(
        functools.partial(leave_kernel, devices),
        out_shape=jax.ShapeDtypeStruct((rows, devices * slots), jnp.bfloat16),
        in_specs=[far, whole],
        out_specs=whole,
        scratch_shapes=[
            pltpu.VMEM((devices, slots, rows), jnp.bfloat16),
            pltpu.SemaphoreType.DMA,
            pltpu.SemaphoreType.DMA((PLANES,)),
            pltpu.SemaphoreType.DMA((PLANES,)),
        ],
        compiler_params=pltpu.CompilerParams(collective_id=1, has_side_effects=True, vmem_limit_bytes=16 << 20),
    )(back, order)


def local(tokens, norm_gain, in_weight, out_weight):
    rows_here = tokens.shape[0]
    channels = in_weight.shape[1]
    devices = lax.axis_size(AXES)
    me = lax.axis_index(AXES)
    slots = channels // devices
    length = rows_here * devices
    inner = 1 << ((length.bit_length()) // 2)
    outer = length // inner
    split = rows_here // inner

    forward, order = channel_tables(slots)
    several = np.eye(channels // PLANES // GROUP_WIDTH)
    forward = np.kron(several, forward.astype(np.float32)).astype(jnp.bfloat16)
    order = np.kron(several, order.astype(np.float32)).T.astype(jnp.bfloat16)
    taken = enter(tokens, norm_gain, in_weight, forward, devices)
    grid = taken.reshape(devices, slots, split, inner).transpose(1, 0, 2, 3)
    zeroth_here = me * (slots // 2) % (GROUP_WIDTH // 2) == 0
    done = position_transform(grid.reshape(slots, outer, inner), zeroth_here, outer, inner)
    back = done.reshape(slots, devices, rows_here // outer, outer).transpose(1, 0, 2, 3)
    ordered = leave(back.reshape(devices, slots, rows_here), order, devices)
    return jnp.dot(ordered, out_weight, preferred_element_type=jnp.float32).astype(jnp.bfloat16)


def solution(mesh):
    placed = (P(AXES, None), P(), P(), P())
    return jax.shard_map(
        local, mesh=mesh, in_specs=placed, out_specs=P(AXES, None), check_vma=False
    )
```

```python
import functools
import math

import jax
import jax.numpy as jnp
import numpy as np
from jax import lax
from jax.experimental import pallas as pl
from jax.experimental.pallas import tpu as pltpu
from jax.sharding import PartitionSpec as P

GROUP_WIDTH = 64
AXES = ("row", "col")


def channel_tables(slots):
    pairs = slots // 2
    half = GROUP_WIDTH // 2
    index = np.arange(GROUP_WIDTH)
    forward = np.zeros((GROUP_WIDTH, GROUP_WIDTH))
    order = np.zeros((GROUP_WIDTH, GROUP_WIDTH))
    for slot in range(GROUP_WIDTH):
        place, within = divmod(slot, slots)
        pair = place * pairs + within % pairs
        angles = 2.0 * math.pi / GROUP_WIDTH * (pair * index % GROUP_WIDTH)
        if within < pairs:
            forward[slot] = np.cos(angles)
            order[pair, slot] = 1.0
        elif pair == 0:
            forward[slot] = np.cos(math.pi * index)
            order[half, slot] = 1.0
        else:
            forward[slot] = np.sin(angles)
            order[GROUP_WIDTH - pair, slot] = 1.0
    forward /= math.sqrt(GROUP_WIDTH)
    return forward.astype(jnp.bfloat16), order.astype(jnp.bfloat16)


def position_tables(outer, inner, devices):
    length = outer * inner
    k1 = np.arange(outer)
    n2 = np.arange(inner)
    n1_order = k1.reshape(devices, -1).T.reshape(-1)
    k2_order = n2.reshape(devices, -1).T.reshape(-1)
    one = 2.0 * math.pi / outer * (np.outer(n1_order, k1) % outer)
    first = np.concatenate([np.cos(one), -np.sin(one)], axis=1)
    turn = 2.0 * math.pi / length * np.outer(n2, k1)
    two = 2.0 * math.pi / inner * (np.outer(k2_order, n2) % inner)
    scale = 1.0 / math.sqrt(length)
    c, s, z = np.cos(two) * scale, np.sin(two) * scale, np.zeros((inner, inner))
    usual = np.block([[c, s, -s, c], [c, s, s, -c]])
    zeroth = np.block([[c, s, z, z], [z, z, c, s]])
    return (
        first.astype(jnp.bfloat16),
        np.cos(turn).astype(np.float32),
        np.sin(turn).astype(np.float32),
        usual.astype(jnp.bfloat16),
        zeroth.astype(jnp.bfloat16),
    )


PLANES = 4
MESH = pl.DeviceIdType.MESH


def place_of(device, columns):
    return (device // columns, device % columns)


def turned_plane(plane, step):
    high = (plane // 2 + 1 - step // 2) % 2
    low = (plane % 2 + (step + 1) // 2) % 2
    return 2 * high + low


def here(devices):
    columns = lax.axis_size("col")
    me = lax.axis_index("row") * columns + lax.axis_index("col")
    per = devices // PLANES
    return me, columns, per, me // per, me % per


def greet(devices):
    me, columns, _, _, _ = here(devices)
    barrier = pltpu.get_barrier_semaphore()

    def signal(step, carry):
        other = (me + step) % devices
        pl.semaphore_signal(barrier, inc=1, device_id=place_of(other, columns), device_id_type=MESH)
        return carry

    lax.fori_loop(1, devices, signal, 0)
    return lambda: pl.semaphore_wait(barrier, devices - 1)


def send_plane(devices, step, from_ref, to_ref, send_sem, recv_sem, first):
    me, columns, per, plane, lane = here(devices)
    target_plane = turned_plane(plane, step)

    def send(hop, carry):
        target = target_plane * per + (lane + hop) % per
        pltpu.make_async_remote_copy(
            src_ref=from_ref.at[target],
            dst_ref=to_ref.at[me],
            send_sem=send_sem,
            recv_sem=recv_sem,
            device_id=place_of(target, columns),
            device_id_type=MESH,
        ).start()
        return carry

    lax.fori_loop(first, per, send, 0)


def wait_for(ref, sem, count):
    part = ref.at[pl.ds(0, count)]
    pltpu.make_async_copy(part, part, sem).wait()


def enter_kernel(
    devices, tokens, gain, weight, forward, out, raw, normed, held, sent, wide, token_sem, weight_sem, own_sem, send_sem, recv_sem
):
    me, columns, per, plane, lane = here(devices)
    pieces = token_sem.shape[0]
    rows = raw.shape[0]
    piece = rows // pieces
    width = held.shape[2]

    def token_copy(index):
        part = pl.ds(index * piece, piece)
        return pltpu.make_async_copy(tokens.at[part], raw.at[part], token_sem.at[index])

    def weight_copy(step):
        target_plane = turned_plane(plane, step)
        part = pl.ds(pl.multiple_of(target_plane * width, width), width)
        return pltpu.make_async_copy(weight.at[:, part], held.at[step], weight_sem.at[step])

    for index in range(pieces):
        token_copy(index).start()
    for step in range(PLANES):
        weight_copy(step).start()
    arrive = greet(devices)

    wide[...] = gain[...].astype(jnp.float32).reshape(wide.shape)
    block = 16
    for index in range(pieces):
        token_copy(index).wait()

        def normalise(number, carry):
            part = pl.ds(pl.multiple_of(index * piece + number * block, block), block)
            floats = raw[part, :].astype(jnp.float32)
            scaling = lax.rsqrt(jnp.mean(floats * floats, axis=-1, keepdims=True) + 1e-06)
            normed[part, :] = (floats * scaling * wide[...]).astype(jnp.bfloat16)
            return carry

        lax.fori_loop(0, piece // block, normalise, 0)

    arrive()

    def chunk(step, carry):
        weight_copy(step).wait()
        target_plane = turned_plane(plane, step)
        hidden = jnp.dot(normed[...], held[step], preferred_element_type=jnp.float32).astype(jnp.bfloat16)
        spectrum = lax.dot_general(
            forward[...], hidden, (((1,), (1,)), ((), ())), preferred_element_type=jnp.float32
        )
        sent[pl.ds(target_plane * per, per)] = spectrum.reshape(per, width // per, rows).astype(jnp.bfloat16)
        send_plane(devices, step, sent, out, send_sem.at[step], recv_sem.at[step], step // (PLANES - 1))
        return carry

    lax.fori_loop(0, PLANES, chunk, 0)
    own = pltpu.make_async_copy(sent.at[me], out.at[me], own_sem)
    own.start()
    finish(per, sent, send_sem)
    finish(per, sent, recv_sem)
    own.wait()


def finish(per, ref, sem):
    for step in range(PLANES):
        wait_for(ref, sem.at[step], per - step // (PLANES - 1))


def enter(tokens, gain, weight, forward, devices):
    rows, depth = tokens.shape
    channels = weight.shape[1]
    slots = channels // devices
    whole = pl.BlockSpec(memory_space=pltpu.VMEM)
    hbm = pl.BlockSpec(memory_space=pltpu.HBM)
    pieces = 4
    return pl.pallas_call(
        functools.partial(enter_kernel, devices),
        out_shape=jax.ShapeDtypeStruct((devices, slots, rows), jnp.bfloat16),
        in_specs=[hbm, whole, hbm, whole],
        out_specs=pl.BlockSpec(memory_space=pl.ANY),
        scratch_shapes=[
            pltpu.VMEM((rows, depth), jnp.bfloat16),
            pltpu.VMEM((rows, depth), jnp.bfloat16),
            pltpu.VMEM((PLANES, depth, channels // PLANES), jnp.bfloat16),
            pltpu.VMEM((devices, slots, rows), jnp.bfloat16),
            pltpu.VMEM((1, depth), jnp.float32),
            pltpu.SemaphoreType.DMA((pieces,)),
            pltpu.SemaphoreType.DMA((PLANES,)),
            pltpu.SemaphoreType.DMA,
            pltpu.SemaphoreType.DMA((PLANES,)),
            pltpu.SemaphoreType.DMA((PLANES,)),
        ],
        compiler_params=pltpu.CompilerParams(collective_id=0, has_side_effects=True, vmem_limit_bytes=61 << 20),
    )(tokens, gain, weight, forward)


def leave_kernel(
    devices,
    taken,
    first,
    turn_cos,
    turn_sin,
    usual,
    special,
    order,
    out,
    table,
    grid,
    done,
    back,
    landed,
    own_sem,
    send_sem,
    recv_sem,
):
    me, columns, per, plane, lane = here(devices)
    arrive = greet(devices)
    units, _, slots, rows = back.shape
    pairs = slots // 2
    outer = first.shape[0]
    inner = turn_cos.shape[0]

    def turned(slot):
        a = lax.dot_general(
            grid[slot], first[...], (((0,), (0,)), ((), ())), preferred_element_type=jnp.float32
        )
        re, im = a[:, :outer], a[:, outer:]
        c, s = turn_cos[...], turn_sin[...]
        return [(re * c + im * s).astype(jnp.bfloat16), (im * c - re * s).astype(jnp.bfloat16)]

    for unit in range(units):
        zeroth_here = ((me * units + unit) * pairs) % (GROUP_WIDTH // 2) == 0

        @pl.when(zeroth_here)
        def _():
            table[...] = special[...]

        @pl.when(jnp.logical_not(zeroth_here))
        def _():
            table[...] = usual[...]

        for part in range(outer // devices):
            block = taken[:, unit * slots : (unit + 1) * slots, part * inner : (part + 1) * inner]
            grid[:, part * devices : (part + 1) * devices, :] = jnp.swapaxes(
                block.astype(jnp.float32), 0, 1
            ).astype(jnp.bfloat16)
        for pair in range(pairs):
            b = jnp.concatenate(turned(pair) + turned(pair + pairs), axis=0)
            here_table = table if pair == 0 else usual
            o = jnp.dot(here_table[...], b, preferred_element_type=jnp.float32)
            done[pair] = o[:inner]
            done[pair + pairs] = o[inner:]
        for part in range(inner // devices):
            block = done[:, part * devices : (part + 1) * devices, :]
            back[unit, :, :, part * outer : (part + 1) * outer] = jnp.swapaxes(block, 0, 1).astype(jnp.bfloat16)
        if unit == 0:
            arrive()
        for step in range(PLANES):
            send_plane(
                devices,
                step,
                back.at[unit],
                landed.at[unit],
                send_sem.at[unit, step],
                recv_sem.at[unit, step],
                step // (PLANES - 1),
            )
        pltpu.make_async_copy(back.at[unit, me], landed.at[unit, me], own_sem.at[unit]).start()

    width = order.shape[0]
    for unit in range(units):
        pltpu.make_async_copy(back.at[unit, me], landed.at[unit, me], own_sem.at[unit]).wait()
    for number in range(PLANES):
        step = PLANES - 1 - number
        source = turned_plane(plane, step)
        parts = []
        for unit in range(units):
            wait_for(landed.at[unit], recv_sem.at[unit, step], per - step // (PLANES - 1))
        for unit in range(units):
            parts.append(landed[unit, pl.ds(source * per, per)].astype(jnp.float32))
        joined = jnp.concatenate(parts, axis=1).reshape(width, rows).astype(jnp.bfloat16)
        turned_back = lax.dot_general(
            joined, order[...], (((0,), (0,)), ((), ())), preferred_element_type=jnp.float32
        ).astype(jnp.bfloat16)
        out[:, pl.ds(pl.multiple_of(source * width, width), width)] = turned_back
    for unit in range(units):
        for step in range(PLANES):
            wait_for(back.at[unit], send_sem.at[unit, step], per - step // (PLANES - 1))


def leave(taken, tables, order, units, devices):
    _, all_slots, rows = taken.shape
    slots = all_slots // units
    outer = tables[0].shape[0]
    inner = tables[1].shape[0]
    whole = pl.BlockSpec(memory_space=pltpu.VMEM)
    return pl.pallas_call(
        functools.partial(leave_kernel, devices),
        out_shape=jax.ShapeDtypeStruct((rows, devices * all_slots), jnp.bfloat16),
        in_specs=[whole] * 7,
        out_specs=whole,
        scratch_shapes=[
            pltpu.VMEM(tables[3].shape, jnp.bfloat16),
            pltpu.VMEM((slots, outer, inner), jnp.bfloat16),
            pltpu.VMEM((slots, inner, outer), jnp.float32),
            pltpu.VMEM((units, devices, slots, rows), jnp.bfloat16),
            pltpu.VMEM((units, devices, slots, rows), jnp.bfloat16),
            pltpu.SemaphoreType.DMA((units,)),
            pltpu.SemaphoreType.DMA((units, PLANES)),
            pltpu.SemaphoreType.DMA((units, PLANES)),
        ],
        compiler_params=pltpu.CompilerParams(collective_id=1, has_side_effects=True, vmem_limit_bytes=20 << 20),
        cost_estimate=pl.CostEstimate(flops=20 * 10**9, bytes_accessed=50 * 2**20, transcendentals=0),
    )(taken, *tables, order)


def local(tokens, norm_gain, in_weight, out_weight):
    rows_here = tokens.shape[0]
    channels = in_weight.shape[1]
    devices = lax.axis_size(AXES)
    slots = channels // devices
    units = max(1, slots // 16)
    length = rows_here * devices
    inner = 1 << ((length.bit_length()) // 2)
    outer = length // inner

    forward, order = channel_tables(slots // units)
    several = np.eye(channels // PLANES // GROUP_WIDTH)
    forward = np.kron(several, forward.astype(np.float32)).astype(jnp.bfloat16)
    order = np.kron(several, order.astype(np.float32)).T.astype(jnp.bfloat16)
    taken = enter(tokens, norm_gain, in_weight, forward, devices)
    ordered = leave(taken, position_tables(outer, inner, devices), order, units, devices)
    return jnp.dot(ordered, out_weight, preferred_element_type=jnp.float32).astype(jnp.bfloat16)


def solution(mesh):
    placed = (P(AXES, None), P(), P(), P())
    return jax.shard_map(
        local, mesh=mesh, in_specs=placed, out_specs=P(AXES, None), check_vma=False
    )
```

```python
import functools
import math

import jax
import jax.numpy as jnp
import numpy as np
from jax import lax
from jax.experimental import pallas as pl
from jax.experimental.pallas import tpu as pltpu
from jax.sharding import PartitionSpec as P

GROUP_WIDTH = 64
AXES = ("row", "col")


def channel_tables(slots):
    pairs = slots // 2
    half = GROUP_WIDTH // 2
    index = np.arange(GROUP_WIDTH)
    forward = np.zeros((GROUP_WIDTH, GROUP_WIDTH))
    order = np.zeros((GROUP_WIDTH, GROUP_WIDTH))
    for slot in range(GROUP_WIDTH):
        place, within = divmod(slot, slots)
        pair = place * pairs + within % pairs
        angles = 2.0 * math.pi / GROUP_WIDTH * (pair * index % GROUP_WIDTH)
        if within < pairs:
            forward[slot] = np.cos(angles)
            order[pair, slot] = 1.0
        elif pair == 0:
            forward[slot] = np.cos(math.pi * index)
            order[half, slot] = 1.0
        else:
            forward[slot] = np.sin(angles)
            order[GROUP_WIDTH - pair, slot] = 1.0
    forward /= math.sqrt(GROUP_WIDTH)
    return forward.astype(jnp.bfloat16), order.astype(jnp.bfloat16)


def position_tables(outer, inner, devices):
    length = outer * inner
    k1 = np.arange(outer)
    n2 = np.arange(inner)
    n1_order = k1.reshape(devices, -1).T.reshape(-1)
    k2_order = n2.reshape(devices, -1).T.reshape(-1)
    one = 2.0 * math.pi / outer * (np.outer(n1_order, k1) % outer)
    first = np.concatenate([np.cos(one), -np.sin(one)], axis=1)
    turn = 2.0 * math.pi / length * np.outer(n2, k1)
    two = 2.0 * math.pi / inner * (np.outer(k2_order, n2) % inner)
    scale = 1.0 / math.sqrt(length)
    c, s, z = np.cos(two) * scale, np.sin(two) * scale, np.zeros((inner, inner))
    usual = np.block([[c, s, -s, c], [c, s, s, -c]])
    zeroth = np.block([[c, s, z, z], [z, z, c, s]])
    return (
        first.astype(jnp.bfloat16),
        np.cos(turn).astype(np.float32),
        np.sin(turn).astype(np.float32),
        usual.astype(jnp.bfloat16),
        zeroth.astype(jnp.bfloat16),
    )


PLANES = 4
MESH = pl.DeviceIdType.MESH


def place_of(device, columns):
    return (device // columns, device % columns)


def turned_plane(plane, step):
    high = (plane // 2 + 1 - step // 2) % 2
    low = (plane % 2 + (step + 1) // 2) % 2
    return 2 * high + low


def here(devices):
    columns = lax.axis_size("col")
    me = lax.axis_index("row") * columns + lax.axis_index("col")
    per = devices // PLANES
    return me, columns, per, me // per, me % per


def greet(devices):
    me, columns, _, _, _ = here(devices)
    barrier = pltpu.get_barrier_semaphore()

    def signal(step, carry):
        other = (me + step) % devices
        pl.semaphore_signal(barrier, inc=1, device_id=place_of(other, columns), device_id_type=MESH)
        return carry

    lax.fori_loop(1, devices, signal, 0)
    return lambda: pl.semaphore_wait(barrier, devices - 1)


def send_plane(devices, step, from_ref, to_ref, send_sem, recv_sem, first):
    me, columns, per, plane, lane = here(devices)
    target_plane = turned_plane(plane, step)

    def send(hop, carry):
        target = target_plane * per + (lane + hop) % per
        pltpu.make_async_remote_copy(
            src_ref=from_ref.at[target],
            dst_ref=to_ref.at[me],
            send_sem=send_sem,
            recv_sem=recv_sem,
            device_id=place_of(target, columns),
            device_id_type=MESH,
        ).start()
        return carry

    lax.fori_loop(first, per, send, 0)


def wait_for(ref, sem, count):
    part = ref.at[pl.ds(0, count)]
    pltpu.make_async_copy(part, part, sem).wait()


def enter_kernel(
    devices, tokens, gain, weight, forward, out, raw, normed, held, sent, wide, token_sem, weight_sem, own_sem, send_sem, recv_sem
):
    me, columns, per, plane, lane = here(devices)
    pieces = token_sem.shape[0]
    rows = raw.shape[0]
    piece = rows // pieces
    width = held.shape[2]

    def token_copy(index):
        part = pl.ds(index * piece, piece)
        return pltpu.make_async_copy(tokens.at[part], raw.at[part], token_sem.at[index])

    def weight_copy(step):
        target_plane = turned_plane(plane, step)
        part = pl.ds(pl.multiple_of(target_plane * width, width), width)
        return pltpu.make_async_copy(weight.at[:, part], held.at[step], weight_sem.at[step])

    for index in range(pieces):
        token_copy(index).start()
    arrive = greet(devices)

    wide[...] = gain[...].astype(jnp.float32).reshape(wide.shape)
    block = 16
    for index in range(pieces):
        token_copy(index).wait()
        weight_copy(index).start()

        def normalise(number, carry):
            part = pl.ds(pl.multiple_of(index * piece + number * block, block), block)
            floats = raw[part, :].astype(jnp.float32)
            scaling = lax.rsqrt(jnp.mean(floats * floats, axis=-1, keepdims=True) + 1e-06)
            normed[part, :] = (floats * scaling * wide[...]).astype(jnp.bfloat16)
            return carry

        lax.fori_loop(0, piece // block, normalise, 0)

    arrive()

    def chunk(step, carry):
        weight_copy(step).wait()
        target_plane = turned_plane(plane, step)
        hidden = jnp.dot(normed[...], held[step], preferred_element_type=jnp.float32).astype(jnp.bfloat16)
        spectrum = lax.dot_general(
            forward[...], hidden, (((1,), (1,)), ((), ())), preferred_element_type=jnp.float32
        )
        sent[pl.ds(target_plane * per, per)] = spectrum.reshape(per, width // per, rows).astype(jnp.bfloat16)
        send_plane(devices, step, sent, out, send_sem.at[step], recv_sem.at[step], step // (PLANES - 1))
        return carry

    lax.fori_loop(0, PLANES, chunk, 0)
    own = pltpu.make_async_copy(sent.at[me], out.at[me], own_sem)
    own.start()
    finish(per, sent, send_sem)
    finish(per, sent, recv_sem)
    own.wait()


def finish(per, ref, sem):
    for step in range(PLANES):
        wait_for(ref, sem.at[step], per - step // (PLANES - 1))


def enter(tokens, gain, weight, forward, devices):
    rows, depth = tokens.shape
    channels = weight.shape[1]
    slots = channels // devices
    whole = pl.BlockSpec(memory_space=pltpu.VMEM)
    hbm = pl.BlockSpec(memory_space=pltpu.HBM)
    pieces = PLANES
    return pl.pallas_call(
        functools.partial(enter_kernel, devices),
        out_shape=jax.ShapeDtypeStruct((devices, slots, rows), jnp.bfloat16),
        in_specs=[hbm, whole, hbm, whole],
        out_specs=pl.BlockSpec(memory_space=pl.ANY),
        scratch_shapes=[
            pltpu.VMEM((rows, depth), jnp.bfloat16),
            pltpu.VMEM((rows, depth), jnp.bfloat16),
            pltpu.VMEM((PLANES, depth, channels // PLANES), jnp.bfloat16),
            pltpu.VMEM((devices, slots, rows), jnp.bfloat16),
            pltpu.VMEM((1, depth), jnp.float32),
            pltpu.SemaphoreType.DMA((pieces,)),
            pltpu.SemaphoreType.DMA((PLANES,)),
            pltpu.SemaphoreType.DMA,
            pltpu.SemaphoreType.DMA((PLANES,)),
            pltpu.SemaphoreType.DMA((PLANES,)),
        ],
        compiler_params=pltpu.CompilerParams(collective_id=0, has_side_effects=True, vmem_limit_bytes=60 << 20),
    )(tokens, gain, weight, forward)


def leave_kernel(
    devices,
    taken,
    first,
    turn_cos,
    turn_sin,
    usual,
    special,
    order,
    out,
    table,
    grid,
    done,
    back,
    landed,
    own_sem,
    send_sem,
    recv_sem,
):
    me, columns, per, plane, lane = here(devices)
    arrive = greet(devices)
    units, _, slots, rows = back.shape
    pairs = slots // 2
    outer = first.shape[0]
    inner = turn_cos.shape[0]

    def turned(slot):
        a = lax.dot_general(
            grid[slot], first[...], (((0,), (0,)), ((), ())), preferred_element_type=jnp.float32
        )
        re, im = a[:, :outer], a[:, outer:]
        c, s = turn_cos[...], turn_sin[...]
        return [(re * c + im * s).astype(jnp.bfloat16), (im * c - re * s).astype(jnp.bfloat16)]

    for unit in range(units):
        zeroth_here = ((me * units + unit) * pairs) % (GROUP_WIDTH // 2) == 0

        @pl.when(zeroth_here)
        def _():
            table[...] = special[...]

        @pl.when(jnp.logical_not(zeroth_here))
        def _():
            table[...] = usual[...]

        for part in range(outer // devices):
            block = taken[:, unit * slots : (unit + 1) * slots, part * inner : (part + 1) * inner]
            grid[:, part * devices : (part + 1) * devices, :] = jnp.swapaxes(
                block.astype(jnp.float32), 0, 1
            ).astype(jnp.bfloat16)
        for pair in range(pairs):
            b = jnp.concatenate(turned(pair) + turned(pair + pairs), axis=0)
            here_table = table if pair == 0 else usual
            o = jnp.dot(here_table[...], b, preferred_element_type=jnp.float32)
            done[pair] = o[:inner]
            done[pair + pairs] = o[inner:]
        for part in range(inner // devices):
            block = done[:, part * devices : (part + 1) * devices, :]
            back[unit, :, :, part * outer : (part + 1) * outer] = jnp.swapaxes(block, 0, 1).astype(jnp.bfloat16)
        if unit == 0:
            arrive()
        for step in range(PLANES):
            send_plane(
                devices,
                step,
                back.at[unit],
                landed.at[unit],
                send_sem.at[unit, step],
                recv_sem.at[unit, step],
                step // (PLANES - 1),
            )
        pltpu.make_async_copy(back.at[unit, me], landed.at[unit, me], own_sem.at[unit]).start()

    width = order.shape[0]
    for unit in range(units):
        pltpu.make_async_copy(back.at[unit, me], landed.at[unit, me], own_sem.at[unit]).wait()
    for number in range(PLANES):
        step = PLANES - 1 - number
        source = turned_plane(plane, step)
        parts = []
        for unit in range(units):
            wait_for(landed.at[unit], recv_sem.at[unit, step], per - step // (PLANES - 1))
        for unit in range(units):
            parts.append(landed[unit, pl.ds(source * per, per)].astype(jnp.float32))
        joined = jnp.concatenate(parts, axis=1).reshape(width, rows).astype(jnp.bfloat16)
        turned_back = lax.dot_general(
            joined, order[...], (((0,), (0,)), ((), ())), preferred_element_type=jnp.float32
        ).astype(jnp.bfloat16)
        out[:, pl.ds(pl.multiple_of(source * width, width), width)] = turned_back
    for unit in range(units):
        for step in range(PLANES):
            wait_for(back.at[unit], send_sem.at[unit, step], per - step // (PLANES - 1))


def leave(taken, tables, order, units, devices):
    _, all_slots, rows = taken.shape
    slots = all_slots // units
    outer = tables[0].shape[0]
    inner = tables[1].shape[0]
    whole = pl.BlockSpec(memory_space=pltpu.VMEM)
    return pl.pallas_call(
        functools.partial(leave_kernel, devices),
        out_shape=jax.ShapeDtypeStruct((rows, devices * all_slots), jnp.bfloat16),
        in_specs=[whole] * 7,
        out_specs=whole,
        scratch_shapes=[
            pltpu.VMEM(tables[3].shape, jnp.bfloat16),
            pltpu.VMEM((slots, outer, inner), jnp.bfloat16),
            pltpu.VMEM((slots, inner, outer), jnp.float32),
            pltpu.VMEM((units, devices, slots, rows), jnp.bfloat16),
            pltpu.VMEM((units, devices, slots, rows), jnp.bfloat16),
            pltpu.SemaphoreType.DMA((units,)),
            pltpu.SemaphoreType.DMA((units, PLANES)),
            pltpu.SemaphoreType.DMA((units, PLANES)),
        ],
        compiler_params=pltpu.CompilerParams(collective_id=1, has_side_effects=True, vmem_limit_bytes=20 << 20),
        cost_estimate=pl.CostEstimate(flops=20 * 10**9, bytes_accessed=50 * 2**20, transcendentals=0),
    )(taken, *tables, order)


def local(tokens, norm_gain, in_weight, out_weight):
    rows_here = tokens.shape[0]
    channels = in_weight.shape[1]
    devices = lax.axis_size(AXES)
    slots = channels // devices
    units = max(1, slots // 16)
    length = rows_here * devices
    inner = 1 << ((length.bit_length()) // 2)
    outer = length // inner

    forward, order = channel_tables(slots // units)
    several = np.eye(channels // PLANES // GROUP_WIDTH)
    forward = np.kron(several, forward.astype(np.float32)).astype(jnp.bfloat16)
    order = np.kron(several, order.astype(np.float32)).T.astype(jnp.bfloat16)
    taken = enter(tokens, norm_gain, in_weight, forward, devices)
    ordered = leave(taken, position_tables(outer, inner, devices), order, units, devices)
    return jnp.dot(ordered, out_weight, preferred_element_type=jnp.float32).astype(jnp.bfloat16)


def solution(mesh):
    placed = (P(AXES, None), P(), P(), P())
    return jax.shard_map(
        local, mesh=mesh, in_specs=placed, out_specs=P(AXES, None), check_vma=False
    )
```
